32 devices in a mesh: fs: 8 (over z, y), tp: 4 (over x, core).
Axes of the slice: x: 2, y: 2, z: 4, core: 2. Of those that a mesh axis runs over, the one named last changes fastest.
Arguments:
- tokens: bfloat16 [8192, 2048], P(('fs', 'tp')), may hold values from -6 to 6
- expert_group: int32 [8192], P(('fs', 'tp')), may hold values from 0 to 1, as said below
- expert_fine: int32 [8192, 2], P(('fs', 'tp')), may hold values from 0 to 3, as said below
- route_weight: float32 [8192, 2], P(('fs', 'tp')), may hold values from 0.2 to 0.9
- norm_gain: float32 [2048], P('fs'), may hold values from 0.1 to 1.9
- gate_master: float32 [8, 2048, 512], P(None, 'fs', 'tp'), may hold values from -0.125 to 0.125
- up_master: float32 [8, 2048, 512], P(None, 'fs', 'tp'), may hold values from -0.125 to 0.125
- down_master: float32 [8, 2048, 512], P(None, 'fs', 'tp'), may hold values from -0.25 to 0.25
Outputs:
- mixed: bfloat16 [8192, 2048], P(('fs', 'tp'))
- gate_ready: bfloat16 [8, 2048, 512], P('fs')
- up_ready: bfloat16 [8, 2048, 512], P('fs')
- down_ready: bfloat16 [8, 2048, 512], P('fs')
The draws below stay inside these ranges and needn't reach their ends.
Inputs may be any that keep to these rules, and one draw needn't show every extreme that they name: `expert_group`: in the rows of one device every group is chosen by the same number of rows. `expert_fine`: the two entries of a row differ. Counting an expert as its group and entry, the rows of one device name one expert at most 128 times, and in every group one expert is named exactly 128 times by the rows of every device.
All inputs are finite; a program needn't handle non-finite values.
Results may differ from the reference program's by a relative error of at most 0.0086.
Values may be sent and summed in bfloat16 or wider, within the bound.
A program may use at most 128 MiB of HBM per device.

```python
import jax
import jax.numpy as jnp
from jax import lax

D = 2048
F = 512
FINE = 4
TOP = 2
TOK_DEV = 256
EXPERTS = 8
GROUPS = 2
CAP = 128
TOKENS = 8192
DEVICES = 32


def route_tables(key):
    base = jax.random.fold_in(key, 7)
    blocks = TOKENS // TOK_DEV
    per_group = TOK_DEV // GROUPS
    pattern = jnp.array([16, 8, 5, 3], jnp.int32)
    hot_key = jax.random.fold_in(base, 1)
    perm_key = jax.random.fold_in(base, 2)
    shuffle_key = jax.random.fold_in(base, 3)
    hot = jax.random.randint(hot_key, (GROUPS,), 0, FINE)
    perms = jax.vmap(lambda sub: jax.random.permutation(sub, FINE))(jax.random.split(perm_key, blocks * GROUPS))
    perms = perms.reshape(blocks, GROUPS, FINE).astype(jnp.int32)
    raw = pattern[perms]
    column = jnp.arange(FINE, dtype=jnp.int32)
    top_pos = jnp.sum(column * (perms == 0).astype(jnp.int32), axis=-1)
    is_hot = column[None, None, :] == hot[None, :, None]
    raw_hot = jnp.sum(raw * is_hot.astype(jnp.int32), axis=-1, keepdims=True)
    weight = jnp.where(is_hot, 16, jnp.where(column[None, None, :] == top_pos[..., None], raw_hot, raw))
    counts = weight * CAP // 16
    bounds = jnp.cumsum(counts, axis=-1)
    within = jnp.arange(per_group, dtype=jnp.int32)
    first = jnp.sum((within[None, None, :, None] >= bounds[:, :, None, :]).astype(jnp.int32), axis=-1)
    second = jnp.sum(((within + per_group)[None, None, :, None] >= bounds[:, :, None, :]).astype(jnp.int32), axis=-1)
    group = jnp.broadcast_to(jnp.arange(GROUPS, dtype=jnp.int32)[None, :, None], first.shape)
    group = group.reshape(blocks, TOK_DEV)
    fine = jnp.stack([first, second], axis=-1).reshape(blocks, TOK_DEV, 2)
    shuffle = jax.vmap(lambda sub: jax.random.permutation(sub, TOK_DEV))(jax.random.split(shuffle_key, blocks)).astype(jnp.int32)
    group = jnp.take_along_axis(group, shuffle, axis=1)
    fine = jnp.take_along_axis(fine, shuffle[:, :, None], axis=1)
    return (group.reshape(TOKENS).astype(jnp.int32), fine.reshape(TOKENS, 2).astype(jnp.int32))


def draw_expert_group(key, part):
    return route_tables(key)[0]


def draw_expert_fine(key, part):
    return route_tables(key)[1]


def shard_levels(stream_key, extent, cuts, low, largest):
    loudness = 1.0
    for dim, parts in cuts:
        steps = jax.random.uniform(jax.random.fold_in(jax.random.fold_in(stream_key, 6), dim), (parts,), jnp.float32, low / len(cuts), largest / len(cuts))
        loudness = loudness * jnp.repeat(jnp.exp(steps), extent[dim] // parts).reshape((-1,) + (1,) * (len(extent) - 1 - dim))
    return loudness


def noise(rng, dims, deviation, most, cuts=(), held_as=jnp.bfloat16):
    loudness = shard_levels(rng, dims, cuts, -0.22, 0.18) if cuts else 1.0
    values = jax.random.normal(rng, dims, jnp.float32) * deviation * loudness
    return jnp.minimum(jnp.maximum(values, -most), most).astype(held_as)


def setup_inputs(seed: int = 0) -> dict:
    key_of = jax.random.split(jax.random.key(seed), 9)
    return {
        "tokens": noise(key_of[0], (TOKENS, D), 1.0, 6.0, ((0, 32),)),
        "expert_group": draw_expert_group(jax.random.fold_in(key_of[8], 71), 0),
        "expert_fine": draw_expert_fine(jax.random.fold_in(key_of[8], 71), 0),
        "route_weight": jnp.clip(0.2 + 0.7 * jax.random.uniform(key_of[3], (TOKENS, TOP), jnp.float32) ** shard_levels(key_of[3], (TOKENS, TOP), ((0, 32),), -0.2, 0.2), 0.2, 0.9),
        "norm_gain": jnp.clip(1.0 + 0.18 * jax.random.normal(key_of[4], (D,), jnp.float32), 0.1, 1.9),
        "gate_master": noise(key_of[5], (EXPERTS, D, F), D ** -0.5, 0.125, ((1, 8), (2, 4)), jnp.float32),
        "up_master": noise(key_of[6], (EXPERTS, D, F), D ** -0.5, 0.125, ((1, 8), (2, 4)), jnp.float32),
        "down_master": noise(key_of[7], (EXPERTS, D, F), F ** -0.5, 0.25, ((1, 8), (2, 4)), jnp.float32),
    }


EPS = 1e-06

def reference(tokens, expert_group, expert_fine, route_weight, norm_gain, gate_master, up_master, down_master):
    gate_ready = (norm_gain[None, :, None] * gate_master).astype(jnp.bfloat16)
    up_ready = (norm_gain[None, :, None] * up_master).astype(jnp.bfloat16)
    down_ready = down_master.astype(jnp.bfloat16)
    widened = tokens.astype(jnp.float32)
    normed = (widened * lax.rsqrt(lax.optimization_barrier(jnp.mean(widened * widened, axis=-1, keepdims=True)) + EPS)).astype(jnp.bfloat16)
    expert = (FINE * expert_group[:, None] + expert_fine).reshape(-1).astype(jnp.int32)
    weights = route_weight.reshape(-1)
    slot_count = DEVICES * CAP

    def per_expert(totals, expert_id):
        hits = expert == expert_id
        chosen = jnp.nonzero(hits, size=slot_count, fill_value=0)[0].astype(jnp.int32)
        filled = jnp.arange(slot_count, dtype=jnp.int32) < jnp.sum(hits.astype(jnp.int32))
        source_row = chosen // TOP
        input_rows = normed[source_row]
        gate_value = jnp.dot(input_rows, gate_ready[expert_id], preferred_element_type=jnp.float32)
        upward = jnp.dot(input_rows, up_ready[expert_id], preferred_element_type=jnp.float32)
        activation = (jax.nn.silu(gate_value) * upward).astype(jnp.bfloat16)
        produced = lax.dot_general(activation, down_ready[expert_id], (((1,), (1,)), ((), ())), preferred_element_type=jnp.float32).astype(jnp.bfloat16)
        scale = jnp.where(filled, weights[chosen], jnp.zeros((), weights.dtype)).astype(jnp.float32)
        totals = totals.at[source_row].add(scale[:, None] * produced.astype(jnp.float32))
        return (totals, None)
    totals, _ = lax.scan(per_expert, jnp.zeros((TOKENS, D), jnp.float32), jnp.arange(EXPERTS, dtype=jnp.int32))
    mixed = totals.astype(jnp.bfloat16)
    return (mixed, gate_ready, up_ready, down_ready)
```

```python
import jax
import jax.numpy as jnp
from jax import lax
from jax.sharding import PartitionSpec as P

FINE = 4


EPS = 1e-06


def flip(value, axis, bit):
    size = lax.axis_size(axis)
    return lax.ppermute(value, axis, [(i, i ^ bit) for i in range(size)])


def shift(value, axis, step):
    size = lax.axis_size(axis)
    return lax.ppermute(value, axis, [(i, (i + step) % size) for i in range(size)])


def place(pieces, positions):
    if len(pieces) == 2:
        return jnp.where(
            positions[0] == 0,
            jnp.concatenate([pieces[0], pieces[1]], axis=-1),
            jnp.concatenate([pieces[1], pieces[0]], axis=-1),
        )
    width = pieces[0].shape[-1]
    whole = jnp.concatenate(pieces, axis=-1)
    for piece, position in zip(pieces, positions):
        whole = lax.dynamic_update_slice_in_dim(whole, piece, position * width, axis=-1)
    return whole


def widen(narrow):
    tp_size = lax.axis_size("tp")
    me = lax.axis_index("tp")
    chips = tp_size // 2
    chip, core = me // 2, me % 2
    cols = narrow.shape[-1]
    pieces = [narrow] + [shift(narrow, "tp", 2 * r) for r in range(1, chips)]
    half = place(pieces, [(chip - r + chips) % chips for r in range(chips)])
    other = flip(half, "tp", 1)
    shape = half.shape[:-1] + (chips, cols)
    mine, theirs = half.reshape(shape), other.reshape(shape)
    both = jnp.where(
        core == 0,
        jnp.stack([mine, theirs], axis=-2),
        jnp.stack([theirs, mine], axis=-2),
    )
    return both.reshape(half.shape[:-1] + (chips * 2 * cols,))


def spread(rows, first, second):
    step = flip(rows, "fs", first)
    pair = jnp.stack([rows, step])
    far = flip(pair, "fs", second)
    return pair, far


def local(
    tokens, expert_group, expert_fine, route_weight, norm_gain, gate_master, up_master, down_master
):
    tok_rows, width = tokens.shape
    fs_size = lax.axis_size("fs")
    experts_all = gate_master.shape[0]
    groups = experts_all // FINE
    members = fs_size // groups
    cap = tok_rows // groups
    fs_me = lax.axis_index("fs")
    group_me, fine_me = fs_me // members, fs_me % members

    widened = tokens.astype(jnp.float32)
    normed = (
        widened * lax.rsqrt(jnp.mean(widened * widened, axis=-1, keepdims=True) + EPS)
    ).astype(jnp.bfloat16)
    away = (expert_group - group_me + groups) % groups
    index = jnp.arange(tok_rows, dtype=jnp.int32)
    same = (away[:, None] == away[None, :]) & (index[None, :] < index[:, None])
    slot = away * cap + jnp.sum(same.astype(jnp.int32), axis=1)
    placing = (index[:, None] == slot[None, :]).astype(jnp.bfloat16)
    ordered = jnp.dot(placing, normed, preferred_element_type=jnp.float32).astype(jnp.bfloat16)
    fines = jnp.arange(FINE, dtype=jnp.int32)
    share = jnp.sum(
        jnp.where(expert_fine[None, :, :] == fines[:, None, None], route_weight[None], 0.0), axis=2
    )
    share = jnp.sum(
        jnp.where((index[:, None] == slot[None, :])[None], share[:, None, :], 0.0), axis=2
    )

    near, near_share = ordered[:cap], share[:, :cap]
    near_x = spread(near, 1, 2)
    near_w = spread(near_share, 1, 2)
    far = jnp.concatenate(
        [shift(ordered[r * cap : (r + 1) * cap], "fs", r * members) for r in range(1, groups)]
    )
    far_share = jnp.concatenate(
        [shift(share[:, r * cap : (r + 1) * cap], "fs", r * members) for r in range(1, groups)],
        axis=1,
    )
    far_x = spread(far, 2, 1)
    far_w = spread(far_share, 2, 1)

    gate_piece = (norm_gain[None, :, None] * gate_master).astype(jnp.bfloat16)
    up_piece = (norm_gain[None, :, None] * up_master).astype(jnp.bfloat16)
    down_piece = down_master.astype(jnp.bfloat16)
    gate_ready, up_ready, down_ready = (
        widen(lax.all_to_all(piece, "fs", split_axis=0, concat_axis=1, tiled=True))
        for piece in (gate_piece, up_piece, down_piece)
    )

    def apply(x_pair, w_pair):
        both, rows = x_pair.shape[0], x_pair.shape[1]
        x = x_pair.reshape(both * rows, width)
        gate_value = jnp.dot(x, gate_ready[0], preferred_element_type=jnp.float32)
        upward = jnp.dot(x, up_ready[0], preferred_element_type=jnp.float32)
        activation = (jax.nn.silu(gate_value) * upward).astype(jnp.bfloat16)
        out = lax.dot_general(
            activation, down_ready[0], (((1,), (1,)), ((), ())), preferred_element_type=jnp.float32
        )
        weight = jnp.sum(
            jnp.where(fines[None, :, None] == fine_me, w_pair, 0.0), axis=1
        )
        return (weight.reshape(both * rows, 1) * out).astype(jnp.bfloat16).reshape(x_pair.shape)

    def collect(xs, ws, first, second):
        far_part = flip(apply(xs[1], ws[1]), "fs", second)
        pair = apply(xs[0], ws[0])
        kept = (pair.astype(jnp.float32) + far_part.astype(jnp.float32)).astype(jnp.bfloat16)
        back = flip(kept[1], "fs", first)
        return (kept[0].astype(jnp.float32) + back.astype(jnp.float32)).astype(jnp.bfloat16)

    far_mixed = collect(far_x, far_w, 2, 1)
    near_mixed = collect(near_x, near_w, 1, 2)
    returned = [near_mixed] + [
        shift(far_mixed[(r - 1) * cap : r * cap], "fs", -r * members) for r in range(1, groups)
    ]
    mixed = lax.dot_general(
        placing,
        jnp.concatenate(returned),
        (((0,), (0,)), ((), ())),
        preferred_element_type=jnp.float32,
    ).astype(jnp.bfloat16)
    return (mixed, gate_ready, up_ready, down_ready)


def solution(mesh):
    in_specs = (
        P(("fs", "tp"), None),
        P(("fs", "tp")),
        P(("fs", "tp"), None),
        P(("fs", "tp"), None),
        P("fs"),
        P(None, "fs", "tp"),
        P(None, "fs", "tp"),
        P(None, "fs", "tp"),
    )
    out_specs = (
        P(("fs", "tp"), None),
        P("fs", None, None),
        P("fs", None, None),
        P("fs", None, None),
    )
    return jax.shard_map(local, mesh=mesh, in_specs=in_specs, out_specs=out_specs, check_vma=False)
```

```python
import functools

import jax
import jax.numpy as jnp
from jax import lax
from jax.experimental import pallas as pl
from jax.experimental.pallas import tpu as pltpu
from jax.sharding import PartitionSpec as P

FINE = 4


EPS = 1e-06


def flip(value, axis, bit):
    size = lax.axis_size(axis)
    return lax.ppermute(value, axis, [(i, i ^ bit) for i in range(size)])


def shift(value, axis, step):
    size = lax.axis_size(axis)
    return lax.ppermute(value, axis, [(i, (i + step) % size) for i in range(size)])


def gather_kernel(
    fs_size, tp_size, members, cap, tok_ref, piece_ref, x_ref, ready_ref,
    local_sem, tsend, trecv, psend, precv, xsend, xrecv, csend, crecv,
):
    groups, chips = fs_size // members, tp_size // 2
    tok_rows = tok_ref.shape[0]
    rows = piece_ref.shape[2]
    fs, tp = lax.axis_index("fs"), lax.axis_index("tp")
    group, member = fs // members, fs % members
    chip, core = tp // 2, tp % 2

    def away(r, i):
        base = member + i - 2 * (member & i)
        ahead = ((group + r) % groups) * members + base
        behind = ((group + groups - r) % groups) * members + base
        return ahead, behind

    def chip_tp(q, c):
        return ((chip + q) % chips) * 2 + c

    peers = [
        (away(r, i)[0], tp) for r in range(groups) for i in range(members) if r or i
    ]
    peers += [(fs, chip_tp(q, core)) for q in range(1, chips)] + [(fs, chip_tp(0, 1 - core))]
    barrier = pltpu.get_barrier_semaphore()
    for f, t in peers:
        pl.semaphore_signal(
            barrier, inc=1, device_id={"fs": f, "tp": t}, device_id_type=pl.DeviceIdType.MESH
        )
    pl.semaphore_wait(barrier, len(peers))

    started = []

    def send(src, dst, send_sem, recv_sem, f, t):
        copy = pltpu.make_async_remote_copy(
            src_ref=src, dst_ref=dst, send_sem=send_sem, recv_sem=recv_sem,
            device_id={"fs": f, "tp": t}, device_id_type=pl.DeviceIdType.MESH,
        )
        copy.start()
        started.append(copy)
        return copy

    near, far = pl.ds(0, cap), pl.ds(cap, tok_rows - cap)

    def pass_on(src, part, j, bit, k):
        return send(
            src, x_ref.at[j, part], tsend.at[k], trecv.at[k], away(0, bit)[0], tp
        )

    def block(f):
        return pl.ds(pl.multiple_of(f * rows, rows), rows)

    near_2 = pass_on(tok_ref.at[near], near, 2, 2, 0)
    near_1 = pass_on(tok_ref.at[near], near, 1, 1, 1)
    crossing = []
    for r in range(1, groups):
        part = pl.ds(r * cap, cap)
        crossing.append(
            send(tok_ref.at[part], x_ref.at[0, part], tsend.at[5 + r], trecv.at[5 + r], away(r, 0)[0], tp)
        )
    kept = pltpu.make_async_copy(tok_ref.at[near], x_ref.at[0, near], local_sem.at[0])
    kept.start()
    own = pltpu.make_async_copy(piece_ref.at[fs], ready_ref.at[tp, :, block(fs)], local_sem.at[1])
    own.start()

    pieces = {}
    for r in range(groups):
        for i in range(members):
            if r or i:
                k = r * members + i
                to = away(r, i)[0]
                pieces[r, i] = send(
                    piece_ref.at[to], ready_ref.at[tp, :, block(fs)], psend.at[k], precv.at[k], to, tp
                )
    own.wait()
    across = {}

    def cross_chips(r, i):
        here = ready_ref.at[tp, :, block(away(r, i)[1])]
        for q in range(1, chips):
            k = r * members + i
            across[q, r, i] = send(
                here, here, xsend.at[q - 1, k], xrecv.at[q - 1, k], fs, chip_tp(q, core)
            )

    beside = []

    def cross_cores(q, r):
        size = members * rows
        start = ((group + groups - r) % groups) * size
        here = ready_ref.at[chip_tp(chips - q, core), :, pl.ds(pl.multiple_of(start, size), size)]
        beside.append(
            send(here, here, csend.at[q, r], crecv.at[q, r], fs, chip_tp(0, 1 - core))
        )

    cross_chips(0, 0)
    for i in range(1, members):
        pieces[0, i].wait_recv()
        cross_chips(0, i)
    cross_cores(0, 0)
    near_2.wait_recv()
    near_3 = pass_on(x_ref.at[2, near], near, 3, 1, 2)
    for copy in crossing:
        copy.wait_recv()
    far_2 = pass_on(x_ref.at[0, far], far, 2, 2, 3)
    far_1 = pass_on(x_ref.at[0, far], far, 1, 1, 4)
    passed = False
    for r in range(1, groups):
        for i in range(members):
            pieces[r, i].wait_recv()
            cross_chips(r, i)
            if not passed and i == members // 2 - 1:
                passed = True
                far_2.wait_recv()
                far_3 = pass_on(x_ref.at[2, far], far, 3, 1, 5)
        cross_cores(0, r)
    for r in range(groups):
        for q in range(1, chips):
            for i in range(members):
                across[q, r, i].wait_recv()
            cross_cores(q, r)
    near_1.wait_recv()
    near_3.wait_recv()
    far_1.wait_recv()
    far_3.wait_recv()
    for copy in beside:
        copy.wait_recv()
    kept.wait()
    for copy in started:
        copy.wait_send()


def gather(ordered, pieces, members, cap):
    fs_size, tp_size = lax.axis_size("fs"), lax.axis_size("tp")
    experts_all, kinds, rows, cols = pieces.shape
    chips = tp_size // 2
    moves, crossings = 6, fs_size // members - 1
    dma = pltpu.SemaphoreType.DMA
    sent = 5 * ordered.size + 3 * pieces.size
    return pl.pallas_call(
        functools.partial(gather_kernel, fs_size, tp_size, members, cap),
        out_shape=(
            jax.ShapeDtypeStruct((members,) + ordered.shape, ordered.dtype),
            jax.ShapeDtypeStruct((tp_size, kinds, fs_size * rows, cols), pieces.dtype),
        ),
        in_specs=[pl.BlockSpec(memory_space=pltpu.VMEM)] * 2,
        out_specs=(pl.BlockSpec(memory_space=pl.ANY),) * 2,
        scratch_shapes=[
            dma((2,)),
            dma((moves + crossings,)),
            dma((moves + crossings,)),
            dma((fs_size,)),
            dma((fs_size,)),
            dma((max(chips - 1, 1), fs_size)),
            dma((max(chips - 1, 1), fs_size)),
            dma((chips, fs_size // members)),
            dma((chips, fs_size // members)),
        ],
        compiler_params=pltpu.CompilerParams(collective_id=0, has_side_effects=True),
        cost_estimate=pl.CostEstimate(flops=0, bytes_accessed=4 * sent, transcendentals=0),
    )(ordered, pieces)


def local(
    tokens, expert_group, expert_fine, route_weight, norm_gain, gate_master, up_master, down_master
):
    tok_rows, width = tokens.shape
    fs_size = lax.axis_size("fs")
    experts_all = gate_master.shape[0]
    groups = experts_all // FINE
    members = fs_size // groups
    cap = tok_rows // groups
    fs_me = lax.axis_index("fs")
    group_me, fine_me = fs_me // members, fs_me % members

    widened = tokens.astype(jnp.float32)
    normed = (
        widened * lax.rsqrt(jnp.mean(widened * widened, axis=-1, keepdims=True) + EPS)
    ).astype(jnp.bfloat16)
    away = (expert_group - group_me + groups) % groups
    index = jnp.arange(tok_rows, dtype=jnp.int32)
    same = (away[:, None] == away[None, :]) & (index[None, :] < index[:, None])
    slot = away * cap + jnp.sum(same.astype(jnp.int32), axis=1)
    placing = (index[:, None] == slot[None, :]).astype(jnp.bfloat16)
    fines = jnp.arange(FINE, dtype=jnp.int32)
    share = jnp.sum(
        jnp.where(expert_fine[:, None, :] == fines[None, :, None], route_weight[:, None, :], 0.0),
        axis=2,
    )
    high = lax.reduce_precision(share, 8, 7)
    middle = lax.reduce_precision(share - high, 8, 7)
    low = share - high - middle
    terms = jnp.concatenate([high, middle, low], axis=1).astype(jnp.bfloat16)
    terms = jnp.pad(terms, ((0, 0), (0, 128 - terms.shape[1])))
    extended = jnp.concatenate([normed, terms], axis=1)
    ordered = jnp.dot(placing, extended, preferred_element_type=jnp.float32).astype(jnp.bfloat16)

    pieces = jnp.stack(
        [norm_gain[None, :, None] * gate_master, norm_gain[None, :, None] * up_master, down_master],
        axis=1,
    ).astype(jnp.bfloat16)
    x_all, ready = gather(ordered, pieces, members, cap)
    gate_ready, up_ready, down_ready = (
        jnp.swapaxes(ready[:, kind], 0, 1).reshape(1, width, -1) for kind in range(3)
    )

    def apply(x_pair):
        both, rows = x_pair.shape[0], x_pair.shape[1]
        flat = x_pair.reshape(both * rows, -1)
        x = flat[:, :width]
        gate_value = jnp.dot(x, gate_ready[0], preferred_element_type=jnp.float32)
        upward = jnp.dot(x, up_ready[0], preferred_element_type=jnp.float32)
        activation = (jax.nn.silu(gate_value) * upward).astype(jnp.bfloat16)
        out = lax.dot_general(
            activation, down_ready[0], (((1,), (1,)), ((), ())), preferred_element_type=jnp.float32
        )
        parts = flat[:, width : width + 3 * FINE].astype(jnp.float32)
        mine = jnp.arange(3 * FINE, dtype=jnp.int32) % FINE == fine_me
        weight = jnp.sum(jnp.where(mine[None, :], parts, 0.0), axis=1, keepdims=True)
        return (weight * out).astype(jnp.bfloat16).reshape(both, rows, width)

    def collect(xs, first, second):
        far_part = flip(apply(jnp.stack([xs[second], xs[first + second]])), "fs", second)
        pair = apply(jnp.stack([xs[0], xs[first]]))
        kept = (pair.astype(jnp.float32) + far_part.astype(jnp.float32)).astype(jnp.bfloat16)
        back = flip(kept[1], "fs", first)
        return (kept[0].astype(jnp.float32) + back.astype(jnp.float32)).astype(jnp.bfloat16)

    far_mixed = collect(x_all[:, cap:], 2, 1)
    near_mixed = collect(x_all[:, :cap], 1, 2)
    returned = [near_mixed] + [
        shift(far_mixed[(r - 1) * cap : r * cap], "fs", -r * members) for r in range(1, groups)
    ]
    mixed = lax.dot_general(
        placing,
        jnp.concatenate(returned),
        (((0,), (0,)), ((), ())),
        preferred_element_type=jnp.float32,
    ).astype(jnp.bfloat16)
    return (mixed, gate_ready, up_ready, down_ready)


def solution(mesh):
    in_specs = (
        P(("fs", "tp"), None),
        P(("fs", "tp")),
        P(("fs", "tp"), None),
        P(("fs", "tp"), None),
        P("fs"),
        P(None, "fs", "tp"),
        P(None, "fs", "tp"),
        P(None, "fs", "tp"),
    )
    out_specs = (
        P(("fs", "tp"), None),
        P("fs", None, None),
        P("fs", None, None),
        P("fs", None, None),
    )
    return jax.shard_map(local, mesh=mesh, in_specs=in_specs, out_specs=out_specs, check_vma=False)
```

```python
import functools

import jax
import jax.numpy as jnp
from jax import lax
from jax.experimental import pallas as pl
from jax.experimental.pallas import tpu as pltpu
from jax.sharding import PartitionSpec as P

FINE = 4


EPS = 1e-06


def flip(value, axis, bit):
    size = lax.axis_size(axis)
    return lax.ppermute(value, axis, [(i, i ^ bit) for i in range(size)])


def shift(value, axis, step):
    size = lax.axis_size(axis)
    return lax.ppermute(value, axis, [(i, (i + step) % size) for i in range(size)])


def gather_kernel(
    fs_size, tp_size, members, cap, tok_ref, piece_ref, x_ref, ready_ref,
    local_sem, tsend, trecv, psend, precv, xsend, xrecv, csend, crecv,
):
    groups, chips = fs_size // members, tp_size // 2
    tok_rows = tok_ref.shape[0]
    rows = piece_ref.shape[2]
    fs, tp = lax.axis_index("fs"), lax.axis_index("tp")
    group, member = fs // members, fs % members
    chip, core = tp // 2, tp % 2

    def away(r, i):
        base = member + i - 2 * (member & i)
        ahead = ((group + r) % groups) * members + base
        behind = ((group + groups - r) % groups) * members + base
        return ahead, behind

    def chip_tp(q, c):
        return ((chip + q) % chips) * 2 + c

    peers = [
        (away(r, i)[0], tp) for r in range(groups) for i in range(members) if r or i
    ]
    peers += [(fs, chip_tp(q, core)) for q in range(1, chips)] + [(fs, chip_tp(0, 1 - core))]
    barrier = pltpu.get_barrier_semaphore()
    for f, t in peers:
        pl.semaphore_signal(
            barrier, inc=1, device_id={"fs": f, "tp": t}, device_id_type=pl.DeviceIdType.MESH
        )
    pl.semaphore_wait(barrier, len(peers))

    started = []

    def send(src, dst, send_sem, recv_sem, f, t):
        copy = pltpu.make_async_remote_copy(
            src_ref=src, dst_ref=dst, send_sem=send_sem, recv_sem=recv_sem,
            device_id={"fs": f, "tp": t}, device_id_type=pl.DeviceIdType.MESH,
        )
        copy.start()
        started.append(copy)
        return copy

    near, far = pl.ds(0, cap), pl.ds(cap, tok_rows - cap)

    def pass_on(src, part, j, bit, k):
        return send(
            src, x_ref.at[j, part], tsend.at[k], trecv.at[k], away(0, bit)[0], tp
        )

    def block(f):
        return pl.ds(pl.multiple_of(f * rows, rows), rows)

    near_2 = pass_on(tok_ref.at[near], near, 2, 2, 0)
    near_1 = pass_on(tok_ref.at[near], near, 1, 1, 1)
    crossing = []
    for r in range(1, groups):
        part = pl.ds(r * cap, cap)
        crossing.append(
            send(tok_ref.at[part], x_ref.at[0, part], tsend.at[5 + r], trecv.at[5 + r], away(r, 0)[0], tp)
        )
    kept = pltpu.make_async_copy(tok_ref.at[near], x_ref.at[0, near], local_sem.at[0])
    kept.start()
    own = pltpu.make_async_copy(piece_ref.at[fs], ready_ref.at[tp, :, block(fs)], local_sem.at[1])
    own.start()

    pieces = {}
    for r in range(groups):
        for i in range(members):
            if r or i:
                k = r * members + i
                to = away(r, i)[0]
                pieces[r, i] = send(
                    piece_ref.at[to], ready_ref.at[tp, :, block(fs)], psend.at[k], precv.at[k], to, tp
                )
    own.wait()
    across = {}

    def cross_chips(r, i):
        here = ready_ref.at[tp, :, block(away(r, i)[1])]
        for q in range(1, chips):
            k = r * members + i
            across[q, r, i] = send(
                here, here, xsend.at[q - 1, k], xrecv.at[q - 1, k], fs, chip_tp(q, core)
            )

    beside = []

    def cross_cores(q, r):
        size = members * rows
        start = ((group + groups - r) % groups) * size
        here = ready_ref.at[chip_tp(chips - q, core), :, pl.ds(pl.multiple_of(start, size), size)]
        beside.append(
            send(here, here, csend.at[q, r], crecv.at[q, r], fs, chip_tp(0, 1 - core))
        )

    cross_chips(0, 0)
    for i in range(1, members):
        pieces[0, i].wait_recv()
        cross_chips(0, i)
    cross_cores(0, 0)
    near_2.wait_recv()
    near_3 = pass_on(x_ref.at[2, near], near, 3, 1, 2)
    for copy in crossing:
        copy.wait_recv()
    far_2 = pass_on(x_ref.at[0, far], far, 2, 2, 3)
    far_1 = pass_on(x_ref.at[0, far], far, 1, 1, 4)
    passed = False
    for r in range(1, groups):
        for i in range(members):
            pieces[r, i].wait_recv()
            cross_chips(r, i)
            if not passed and i == members // 2 - 1:
                passed = True
                far_2.wait_recv()
                far_3 = pass_on(x_ref.at[2, far], far, 3, 1, 5)
        cross_cores(0, r)
    for r in range(groups):
        for q in range(1, chips):
            for i in range(members):
                across[q, r, i].wait_recv()
            cross_cores(q, r)
    near_1.wait_recv()
    near_3.wait_recv()
    far_1.wait_recv()
    far_3.wait_recv()
    for copy in beside:
        copy.wait_recv()
    kept.wait()
    for copy in started:
        copy.wait_send()


def gather(ordered, pieces, members, cap):
    fs_size, tp_size = lax.axis_size("fs"), lax.axis_size("tp")
    experts_all, kinds, rows, cols = pieces.shape
    chips = tp_size // 2
    moves, crossings = 6, fs_size // members - 1
    dma = pltpu.SemaphoreType.DMA
    sent = 5 * ordered.size + 3 * pieces.size
    return pl.pallas_call(
        functools.partial(gather_kernel, fs_size, tp_size, members, cap),
        out_shape=(
            jax.ShapeDtypeStruct((members,) + ordered.shape, ordered.dtype),
            jax.ShapeDtypeStruct((tp_size, kinds, fs_size * rows, cols), pieces.dtype),
        ),
        in_specs=[pl.BlockSpec(memory_space=pltpu.VMEM)] * 2,
        out_specs=(pl.BlockSpec(memory_space=pl.ANY),) * 2,
        scratch_shapes=[
            dma((2,)),
            dma((moves + crossings,)),
            dma((moves + crossings,)),
            dma((fs_size,)),
            dma((fs_size,)),
            dma((max(chips - 1, 1), fs_size)),
            dma((max(chips - 1, 1), fs_size)),
            dma((chips, fs_size // members)),
            dma((chips, fs_size // members)),
        ],
        compiler_params=pltpu.CompilerParams(collective_id=0, has_side_effects=True),
        cost_estimate=pl.CostEstimate(flops=0, bytes_accessed=4 * sent, transcendentals=0),
    )(ordered, pieces)


def apply_rows(x_ref, mine_ref, gate_ref, up_ref, down_ref, kept_ref, sent_ref, kept_at, sent_at):
    members, cap, _ = x_ref.shape
    width, _ = gate_ref.shape
    x = x_ref[:, :, :width].reshape(members * cap, width)
    parts = x_ref[:, :, width:].reshape(members * cap, -1).astype(jnp.float32)
    weight = jnp.sum(parts * mine_ref[...], axis=1, keepdims=True)
    gate_value = jnp.dot(x, gate_ref[...], preferred_element_type=jnp.float32)
    upward = jnp.dot(x, up_ref[...], preferred_element_type=jnp.float32)
    activation = (gate_value / (1.0 + jnp.exp(-gate_value)) * upward).astype(jnp.bfloat16)
    step = min(width, 512)
    for at in range(0, width, step):
        out = lax.dot_general(
            activation,
            down_ref[at : at + step, :],
            (((1,), (1,)), ((), ())),
            preferred_element_type=jnp.float32,
        )
        out = (weight * out).astype(jnp.bfloat16)
        for ref, places in ((kept_ref, kept_at), (sent_ref, sent_at)):
            for i, j in enumerate(places):
                ref[i, :, at : at + step] = out[j * cap : (j + 1) * cap]


def first_kernel(kept_at, sent_at, x_ref, mine_ref, ready_ref, kept_ref, sent_ref, *whole_refs):
    @pl.when(pl.program_id(0) == 0)
    def _():
        cols = ready_ref.shape[3]
        for kind, ref in enumerate(whole_refs):
            for t in range(ready_ref.shape[0]):
                ref[0, :, t * cols : (t + 1) * cols] = ready_ref[t, kind]

    apply_rows(
        x_ref, mine_ref, *(ref.at[0] for ref in whole_refs), kept_ref, sent_ref, kept_at, sent_at
    )


def second_kernel(kept_at, sent_at, x_ref, mine_ref, gate_ref, up_ref, down_ref, kept_ref, sent_ref):
    apply_rows(
        x_ref, mine_ref, gate_ref.at[0], up_ref.at[0], down_ref.at[0],
        kept_ref, sent_ref, kept_at, sent_at,
    )


def expert_rows(x_all, mine, weights, cap, first_block, blocks, kept_at, sent_at):
    members, _, extended = x_all.shape
    gathered = len(weights) == 1
    if gathered:
        tp_size, kinds, width, cols = weights[0].shape
        whole = (1, width, tp_size * cols)
    else:
        whole = weights[0].shape
        width = whole[1]

    def fixed(shape):
        return pl.BlockSpec(shape, lambda i: (0,) * len(shape))

    half = jax.ShapeDtypeStruct((members // 2, blocks * cap, width), jnp.bfloat16)
    half_spec = pl.BlockSpec((members // 2, cap, width), lambda i: (0, i, 0))
    extra = 3 if gathered else 0
    body = functools.partial(first_kernel if gathered else second_kernel, kept_at, sent_at)
    hidden = whole[2]
    return pl.pallas_call(
        body,
        grid=(blocks,),
        in_specs=[
            pl.BlockSpec((members, cap, extended), lambda i: (0, i + first_block, 0)),
            fixed(mine.shape),
        ]
        + [fixed(w.shape) for w in weights],
        out_specs=[half_spec] * 2 + [fixed(whole)] * extra,
        out_shape=[half] * 2 + [jax.ShapeDtypeStruct(whole, jnp.bfloat16)] * extra,
        compiler_params=pltpu.CompilerParams(vmem_limit_bytes=56 << 20),
        cost_estimate=pl.CostEstimate(
            flops=6 * members * blocks * cap * width * hidden,
            bytes_accessed=2 * (6 * width * hidden + 2 * members * blocks * cap * width),
            transcendentals=members * blocks * cap * hidden,
        ),
    )(x_all, mine, *weights)


def local(
    tokens, expert_group, expert_fine, route_weight, norm_gain, gate_master, up_master, down_master
):
    tok_rows, width = tokens.shape
    fs_size = lax.axis_size("fs")
    experts_all = gate_master.shape[0]
    groups = experts_all // FINE
    members = fs_size // groups
    cap = tok_rows // groups
    fs_me = lax.axis_index("fs")
    group_me, fine_me = fs_me // members, fs_me % members

    widened = tokens.astype(jnp.float32)
    normed = (
        widened * lax.rsqrt(jnp.mean(widened * widened, axis=-1, keepdims=True) + EPS)
    ).astype(jnp.bfloat16)
    away = (expert_group - group_me + groups) % groups
    index = jnp.arange(tok_rows, dtype=jnp.int32)
    same = (away[:, None] == away[None, :]) & (index[None, :] < index[:, None])
    slot = away * cap + jnp.sum(same.astype(jnp.int32), axis=1)
    placing = (index[:, None] == slot[None, :]).astype(jnp.bfloat16)
    fines = jnp.arange(FINE, dtype=jnp.int32)
    share = jnp.sum(
        jnp.where(expert_fine[:, None, :] == fines[None, :, None], route_weight[:, None, :], 0.0),
        axis=2,
    )
    high = lax.reduce_precision(share, 8, 7)
    middle = lax.reduce_precision(share - high, 8, 7)
    low = share - high - middle
    terms = jnp.concatenate([high, middle, low], axis=1).astype(jnp.bfloat16)
    terms = jnp.pad(terms, ((0, 0), (0, 128 - terms.shape[1])))
    extended = jnp.concatenate([normed, terms], axis=1)
    ordered = jnp.dot(placing, extended, preferred_element_type=jnp.float32).astype(jnp.bfloat16)

    pieces = jnp.stack(
        [norm_gain[None, :, None] * gate_master, norm_gain[None, :, None] * up_master, down_master],
        axis=1,
    ).astype(jnp.bfloat16)
    x_all, ready = gather(ordered, pieces, members, cap)
    lanes = jnp.arange(128, dtype=jnp.int32)
    mine = ((lanes % FINE == fine_me) & (lanes < 3 * FINE)).astype(jnp.float32)[None, :]

    def collect(kept, sent, first, second):
        far_part = flip(sent, "fs", second)
        pair = (kept.astype(jnp.float32) + far_part.astype(jnp.float32)).astype(jnp.bfloat16)
        back = flip(pair[1], "fs", first)
        return (pair[0].astype(jnp.float32) + back.astype(jnp.float32)).astype(jnp.bfloat16)

    kept, sent, gate_ready, up_ready, down_ready = expert_rows(
        x_all, mine, (ready,), cap, 1, groups - 1, (0, 2), (1, 3)
    )
    far_mixed = collect(kept, sent, 2, 1)
    kept, sent = expert_rows(
        x_all, mine, (gate_ready, up_ready, down_ready), cap, 0, 1, (0, 1), (2, 3)
    )
    near_mixed = collect(kept, sent, 1, 2)
    returned = [near_mixed] + [
        shift(far_mixed[(r - 1) * cap : r * cap], "fs", -r * members) for r in range(1, groups)
    ]
    mixed = lax.dot_general(
        placing,
        jnp.concatenate(returned),
        (((0,), (0,)), ((), ())),
        preferred_element_type=jnp.float32,
    ).astype(jnp.bfloat16)
    return (mixed, gate_ready, up_ready, down_ready)


def solution(mesh):
    in_specs = (
        P(("fs", "tp"), None),
        P(("fs", "tp")),
        P(("fs", "tp"), None),
        P(("fs", "tp"), None),
        P("fs"),
        P(None, "fs", "tp"),
        P(None, "fs", "tp"),
        P(None, "fs", "tp"),
    )
    out_specs = (
        P(("fs", "tp"), None),
        P("fs", None, None),
        P("fs", None, None),
        P("fs", None, None),
    )
    return jax.shard_map(local, mesh=mesh, in_specs=in_specs, out_specs=out_specs, check_vma=False)
```
